256 devices in a mesh: fs: 32 (over z, y), tp: 8 (over x, core).
Axes of the slice: x: 4, y: 4, z: 8, core: 2. Of those that a mesh axis runs over, the one named last changes fastest.
Arguments:
- tokens: bfloat16 [8192, 2048], P('fs'), may hold values from -6 to 6
- routes: int32 [8192, 6], P('fs'), may hold values from 0 to 31, all different within a row; in each aligned block of 256 rows (0 to 255, 256 to 511, ...) at most 80 rows name the same one
- route_weights: float32 [8192, 6], P('fs'), may hold values from 0.1 to 1
- norm_gain: float32 [2048], P('fs'), may hold values from 0.1 to 1.9
- expert_gate: float32 [32, 2048, 1024], P(None, 'fs', 'tp'), may hold values from -0.125 to 0.125
- expert_up: float32 [32, 2048, 1024], P(None, 'fs', 'tp'), may hold values from -0.125 to 0.125
- expert_down: float32 [32, 2048, 1024], P(None, 'fs', 'tp'), may hold values from -0.1875 to 0.1875
- shared_gate: float32 [2048, 1024], P('fs', 'tp'), may hold values from -0.125 to 0.125
- shared_up: float32 [2048, 1024], P('fs', 'tp'), may hold values from -0.125 to 0.125
- shared_down: float32 [2048, 1024], P('fs', 'tp'), may hold values from -0.1875 to 0.1875
Outputs:
- layer_output: bfloat16 [8192, 2048], P('fs', 'tp')
- sample_gate: bfloat16 [32, 2048, 1024], P('fs', None, 'tp')
- sample_up: bfloat16 [32, 2048, 1024], P('fs', None, 'tp')
- sample_down: bfloat16 [32, 2048, 1024], P('fs', None, 'tp')
- common_gate: bfloat16 [2048, 1024], P(None, 'tp')
- common_up: bfloat16 [2048, 1024], P(None, 'tp')
- common_down: bfloat16 [2048, 1024], P(None, 'tp')
The draws below stay inside these ranges and needn't reach their ends.
Inputs may be any that keep to these rules, and one draw needn't show every extreme that they name: `routes`: each row names 6 different experts. In each aligned block of 256 rows (the rows of one index of fs) no expert is named by more than 80 rows, a bound that some expert reaches in some blocks.
All inputs are finite; a program needn't handle non-finite values.
Results may differ from the reference program's by a relative error of at most 0.015.
Values may be sent and summed in bfloat16 or wider, within the bound.
A program may use at most 128 MiB of HBM per device.

```python
import math
import jax
import jax.numpy as jnp
import numpy as np
from jax import lax

D = 2048
FF = 1024
SH = 1024
TOP = 6
TOK_DEV = 256
EXPERTS = 32
CAP = 80
TOKENS = 8192
N_FS = 32
N_TP = 8


def block_scale(stream_key, dims, split, least, high):
    gain = 1.0
    for dim, blocks in split:
        draws = jax.random.uniform(jax.random.fold_in(jax.random.fold_in(stream_key, 6), dim), (blocks,), jnp.float32, least / len(split), high / len(split))
        gain = gain * jnp.repeat(jnp.exp(draws), dims[dim] // blocks).reshape((-1,) + (1,) * (len(dims) - 1 - dim))
    return gain


def deal_out(key, own, number, rows, count, top, bound, slope):
    ranking = jax.random.permutation(key, count)
    heavy_load, ordinary = shares(count, rows * top, bound, slope, True), shares(count, rows * top, bound, slope, False)
    places = jnp.arange(count)

    def named(tallies, rotation):
        used = int((tallies > 0).sum())
        fixed = max(1, used // 4)
        shifted = fixed + (places - fixed + rotation * (used - fixed)) % max(1, count - fixed)
        return jnp.zeros((count,), jnp.int32).at[ranking[jnp.where(places < fixed, places, shifted)]].set(jnp.asarray(tallies, jnp.int32))

    tallies = jnp.where(number % 4 == 0, named(heavy_load, number // 4), named(ordinary, number - number // 4 - 1))
    mixed = jax.random.permutation(jax.random.fold_in(own, 3), count)
    giver, taker = mixed[0:count // 2 * 2:2], mixed[1:count // 2 * 2:2]
    room = jnp.minimum(tallies[giver] - 1, bound - tallies[taker]) // 2
    room = jnp.where((giver == ranking[0]) | (taker == ranking[0]) | (tallies[taker] == 0), 0, jnp.maximum(room, 0))
    shifted = jax.random.randint(jax.random.fold_in(own, 4), (count // 2,), 0, 1 << 20) % (room + 1)
    tallies = tallies.at[giver].add(-shifted).at[taker].add(shifted)
    items = jnp.searchsorted(jnp.cumsum(tallies), jnp.arange(rows * top), side="right").astype(jnp.int32)
    table = items.reshape(top, rows).T
    table = table[jax.random.permutation(jax.random.fold_in(own, 1), rows)]
    rotation = jax.random.randint(jax.random.fold_in(own, 2), (rows, 1), 0, top)
    return jnp.take_along_axis(table, (jnp.arange(top)[None, :] + rotation) % top, axis=1)


def shares(number_of, total, limit, slope, full):
    portions = [(1 << 20) // math.isqrt(grade ** slope) + 1 for grade in range(1, number_of + 1)]
    largest = limit if full else min(limit, max(-(-total // number_of), total * portions[0] // sum(portions)))
    least = 1 if total - largest >= number_of - 1 else 0
    counts, rest = [largest] + [least] * (number_of - 1), total - largest - least * (number_of - 1)
    while rest > 0:
        free = [i for i in range(1, number_of) if counts[i] < largest] or [i for i in range(1, number_of) if counts[i] < limit]
        pool, budget = sum([portions[i] for i in free]), rest
        for i in free:
            extra = min(limit - counts[i], max(1, budget * portions[i] // pool), rest)
            counts[i] = counts[i] + extra
            rest = rest - extra
    return np.array(counts)


def normal_values(stream_key, shape, scale, limit, shards=(), kind=jnp.bfloat16):
    result = scale * jax.random.normal(stream_key, shape, jnp.float32)
    if shards:
        result = result * block_scale(stream_key, shape, shards, -0.22, 0.18)
    return jnp.clip(result, -limit, limit).astype(kind)


def setup_inputs(seed: int = 0) -> dict:
    streams_of = jax.random.split(jax.random.key(seed), 11)
    tokens = normal_values(streams_of[0], (TOKENS, D), 1.0, 6.0, ((0, 32),))
    routes_keys = jax.random.split(jax.random.fold_in(streams_of[1], 1), TOKENS // TOK_DEV)
    routes_turns = jax.random.permutation(jax.random.fold_in(streams_of[1], 3), TOKENS // TOK_DEV)
    routes = jax.vmap(lambda own, number: deal_out(jax.random.fold_in(streams_of[1], 2), own, number, TOK_DEV, EXPERTS, TOP, CAP, 1))(routes_keys, routes_turns).reshape((TOKENS, TOP))
    route_weights = jnp.clip(jnp.exp(math.log(1.0) - 2.3025851 * jax.random.uniform(streams_of[2], (TOKENS, TOP), jnp.float32) ** block_scale(streams_of[2], (TOKENS, TOP), ((0, 32),), -0.2, 0.2)), 0.1, 1.0)
    norm_gain = jnp.clip(1.0 + 0.18 * jax.random.normal(streams_of[3], (D,), jnp.float32), 0.1, 1.9)
    expert_gate = normal_values(streams_of[4], (EXPERTS, D, FF), D ** -0.5, 0.125, ((1, 32), (2, 8)), jnp.float32)
    expert_up = normal_values(streams_of[5], (EXPERTS, D, FF), D ** -0.5, 0.125, ((1, 32), (2, 8)), jnp.float32)
    expert_down = normal_values(streams_of[6], (EXPERTS, D, FF), FF ** -0.5, 0.1875, ((1, 32), (2, 8)), jnp.float32)
    shared_gate = normal_values(streams_of[7], (D, SH), D ** -0.5, 0.125, ((0, 32), (1, 8)), jnp.float32)
    shared_up = normal_values(streams_of[8], (D, SH), D ** -0.5, 0.125, ((0, 32), (1, 8)), jnp.float32)
    shared_down = normal_values(streams_of[9], (D, SH), SH ** -0.5, 0.1875, ((0, 32), (1, 8)), jnp.float32)
    return dict(tokens=tokens, routes=routes, route_weights=route_weights, norm_gain=norm_gain, expert_gate=expert_gate, expert_up=expert_up, expert_down=expert_down, shared_gate=shared_gate, shared_up=shared_up, shared_down=shared_down)


EPSILON = 1e-06

def normalize(tokens):
    values = tokens.astype(jnp.float32)
    scale = lax.rsqrt(lax.optimization_barrier(jnp.mean(values * values, axis=-1, keepdims=True)) + EPSILON)
    return (values * scale).astype(jnp.bfloat16)

def block_sum(hidden, down):
    block_width = hidden.shape[1] // N_TP
    total = jnp.zeros((hidden.shape[0], down.shape[0]), jnp.float32)
    for block in range(N_TP):
        lower = block * block_width
        part = jnp.dot(hidden[:, lower:lower + block_width], down[:, lower:lower + block_width].T, preferred_element_type=jnp.float32).astype(jnp.bfloat16)
        part = lax.optimization_barrier(part)
        total = total + part.astype(jnp.float32)
    return total

def reference(tokens, routes, route_weights, norm_gain, expert_gate, expert_up, expert_down, shared_gate, shared_up, shared_down):
    sample_gate = (norm_gain[None, :, None] * expert_gate).astype(jnp.bfloat16)
    sample_up = (norm_gain[None, :, None] * expert_up).astype(jnp.bfloat16)
    sample_down = expert_down.astype(jnp.bfloat16)
    common_gate = (norm_gain[:, None] * shared_gate).astype(jnp.bfloat16)
    common_up = (norm_gain[:, None] * shared_up).astype(jnp.bfloat16)
    common_down = shared_down.astype(jnp.bfloat16)
    normed = normalize(tokens)
    route_blocks = routes.reshape(N_FS, TOK_DEV * TOP)
    member = (route_blocks[:, :, None] == jnp.arange(EXPERTS, dtype=jnp.int32)[None, None, :]).astype(jnp.int32)
    before = lax.optimization_barrier(jnp.sum((jnp.cumsum(member, axis=1) - member) * member, axis=2))
    block_index = jnp.arange(N_FS, dtype=jnp.int32)[:, None]
    slots = (route_blocks * (N_FS * CAP) + block_index * CAP + before).reshape(-1)
    row_index = (block_index * TOK_DEV + jnp.arange(TOK_DEV * TOP, dtype=jnp.int32)[None, :] // TOP).reshape(-1)
    sources = jnp.full((EXPERTS * N_FS * CAP,), TOKENS, jnp.int32).at[slots].set(row_index)
    padded = jnp.concatenate([normed, jnp.zeros((1, D), jnp.bfloat16)], axis=0)

    def per_expert(operands):
        expert_rows, gate_w, up_w, down_w = operands
        rows = padded[expert_rows]
        gate = jnp.dot(rows, gate_w, preferred_element_type=jnp.float32)
        upward = jnp.dot(rows, up_w, preferred_element_type=jnp.float32)
        hidden = (jax.nn.silu(gate) * upward).astype(jnp.bfloat16)
        return block_sum(hidden, down_w).astype(jnp.bfloat16)
    expert_out = lax.map(per_expert, (sources.reshape(EXPERTS, N_FS * CAP), sample_gate, sample_up, sample_down))
    picked = expert_out.reshape(EXPERTS * N_FS * CAP, D)[slots].astype(jnp.float32).reshape(TOKENS, TOP, D)
    routed = lax.optimization_barrier(jnp.sum(picked * route_weights[:, :, None], axis=1))
    shared_gate_act = jnp.dot(normed, common_gate, preferred_element_type=jnp.float32)
    shared_up_act = jnp.dot(normed, common_up, preferred_element_type=jnp.float32)
    shared_hidden = (jax.nn.silu(shared_gate_act) * shared_up_act).astype(jnp.bfloat16)
    shared_sum = block_sum(shared_hidden, common_down)
    layer_output = (routed + shared_sum).astype(jnp.bfloat16)
    return (layer_output, sample_gate, sample_up, sample_down, common_gate, common_up, common_down)
```

```python
import jax
import jax.numpy as jnp
from jax import lax
from jax.sharding import PartitionSpec as P

EPSILON = 1e-06


def normalize(tokens):
    values = tokens.astype(jnp.float32)
    scale = lax.rsqrt(jnp.mean(values * values, axis=-1, keepdims=True) + EPSILON)
    return (values * scale).astype(jnp.bfloat16)


def body(
    tokens,
    routes,
    route_weights,
    norm_gain,
    expert_gate,
    expert_up,
    expert_down,
    shared_gate,
    shared_up,
    shared_down,
):
    bf16, f32 = jnp.bfloat16, jnp.float32
    tp_count = lax.axis_size("tp")
    me_tp = lax.axis_index("tp")
    experts = expert_gate.shape[0]
    gain_rows = norm_gain[None, :, None]
    packed = jnp.concatenate(
        [
            (expert_gate * gain_rows).astype(bf16),
            (expert_up * gain_rows).astype(bf16),
            expert_down.astype(bf16),
        ],
        axis=2,
    )
    mine = lax.all_to_all(packed, "fs", split_axis=0, concat_axis=1, tiled=True)
    width = expert_gate.shape[2]
    sample_gate, sample_up, sample_down = (
        mine[:, :, i * width : (i + 1) * width] for i in range(3)
    )
    normed = normalize(tokens)
    tok_rows, depth = normed.shape
    share = tok_rows // tp_count
    hits = routes[:, :, None] == jnp.arange(experts, dtype=jnp.int32)[None, None, :]
    dense = jnp.sum(jnp.where(hits, route_weights[:, :, None], 0.0), axis=1)
    own_rows = lax.dynamic_slice_in_dim(normed, me_tp * share, share, 0)
    own_dense = lax.dynamic_slice_in_dim(dense, me_tp * share, share, 0)
    rows = lax.all_gather(own_rows, "fs", axis=0, tiled=True)
    scales = lax.all_to_all(own_dense.T, "fs", split_axis=0, concat_axis=0, tiled=True)
    scales = scales.reshape(-1, 1)

    shared_packed = jnp.concatenate(
        [
            (shared_gate * norm_gain[:, None]).astype(bf16),
            (shared_up * norm_gain[:, None]).astype(bf16),
            shared_down.astype(bf16),
        ],
        axis=1,
    )
    common = lax.all_gather(shared_packed, "fs", axis=0, tiled=True)
    common_gate, common_up, common_down = (
        common[:, i * width : (i + 1) * width] for i in range(3)
    )
    sg = jnp.dot(normed, common_gate, preferred_element_type=f32)
    su = jnp.dot(normed, common_up, preferred_element_type=f32)
    sh = (jax.nn.silu(sg) * su).astype(bf16)
    shared_terms = jnp.einsum("th,dh->td", sh, common_down, preferred_element_type=f32).astype(bf16)
    shared_sum = lax.psum_scatter(shared_terms, "tp", scatter_dimension=0, tiled=True)

    whole = lax.all_gather(mine[0], "tp", axis=0, tiled=False)
    total = jnp.zeros((), f32)
    gate = jnp.einsum("rd,bdh->rbh", rows, whole[:, :, :width], preferred_element_type=f32)
    up = jnp.einsum("rd,bdh->rbh", rows, whole[:, :, width : 2 * width], preferred_element_type=f32)
    hidden = (jax.nn.silu(gate) * up).astype(bf16)
    out = jnp.einsum("rbh,bdh->rd", hidden, whole[:, :, 2 * width :], preferred_element_type=f32)
    weighted = (out * scales).astype(bf16)
    routed = lax.psum_scatter(weighted, "fs", scatter_dimension=0, tiled=True)
    final = (routed.astype(f32) + shared_sum.astype(f32)).astype(bf16)
    layer_output = lax.all_to_all(final, "tp", split_axis=1, concat_axis=0, tiled=True)
    return (layer_output, sample_gate, sample_up, sample_down, common_gate, common_up, common_down)


def solution(mesh):
    return jax.shard_map(
        body,
        mesh=mesh,
        in_specs=(
            P("fs", None),
            P("fs", None),
            P("fs", None),
            P("fs"),
            P(None, "fs", "tp"),
            P(None, "fs", "tp"),
            P(None, "fs", "tp"),
            P("fs", "tp"),
            P("fs", "tp"),
            P("fs", "tp"),
        ),
        out_specs=(
            P("fs", "tp"),
            P("fs", None, "tp"),
            P("fs", None, "tp"),
            P("fs", None, "tp"),
            P(None, "tp"),
            P(None, "tp"),
            P(None, "tp"),
        ),
        check_vma=False,
    )
```

```python
import functools
import jax
import jax.numpy as jnp
from jax import lax
from jax.experimental import pallas as pl
from jax.experimental.pallas import tpu as pltpu
from jax.sharding import PartitionSpec as P

MESH = pl.DeviceIdType.MESH
bf16, f32 = jnp.bfloat16, jnp.float32
NZ, NY, NX = 8, 4, 4
COLS = 2048 + 128

A2A = 0
TOKZ = 3
TOKY = 11
SHZ = 15
SHY = 23
XAG = 27
RAZ = 54
RAY = 62
RBY = 66
RBZ = 70
SPX = 78
FIN = 79
NSEM = 80


def rc(src, dst, ssem, rsem, dev):
    return pltpu.make_async_remote_copy(
        src_ref=src, dst_ref=dst, send_sem=ssem, recv_sem=rsem, device_id=dev, device_id_type=MESH
    )


def kernel(
    tok_ref, dense_ref, gain_ref, eg_ref, eu_ref, ed_ref, sg_ref, su_ref, sd_ref,
    lo_out, sg_out, su_out, sd_out, cm_out,
    wsend, w, tk, sh, nb, gbuf, hbuf, ob, ra, ya, yb, zb, sa, sp, sr, fin, lo, send, recv, loc,
):
    fs, tp = lax.axis_index("fs"), lax.axis_index("tp")
    z, y = fs // NY, fs % NY
    x, c = tp // 2, tp % 2

    def at_z(d):
        return ((z + d + NZ) % NZ) * NY + y

    def at_y(d):
        return z * NY + (y + d + NY) % NY

    xr, xl = ((x + 1) % NX) * 2 + c, ((x + NX - 1) % NX) * 2 + c
    mate = x * 2 + 1 - c

    barrier = pltpu.get_barrier_semaphore()

    def sig_fs(i, _):
        pl.semaphore_signal(barrier, inc=1, device_id=((fs + i) % 32, tp), device_id_type=MESH)
        return 0

    def sig_tp(i, _):
        pl.semaphore_signal(barrier, inc=1, device_id=(fs, (tp + i) % 8), device_id_type=MESH)
        return 0

    lax.fori_loop(1, 32, sig_fs, 0)
    lax.fori_loop(1, 8, sig_tp, 0)

    rows = tok_ref[pl.ds(pl.multiple_of(tp * 32, 32), 32), :].astype(f32)
    scale = lax.rsqrt(jnp.mean(rows * rows, axis=-1, keepdims=True) + 1e-6)
    yrow = pl.multiple_of(y * 32, 32)
    tk[z, pl.ds(yrow, 32), 0:2048] = (rows * scale).astype(bf16)
    tk[z, pl.ds(yrow, 32), 2048:2176] = dense_ref[pl.ds(pl.multiple_of(tp * 32, 32), 32), :]
    gain = gain_ref[...]
    yr64 = pl.multiple_of(y * 64, 64)
    sh[0, z, pl.ds(yr64, 64), :] = (sg_ref[...] * gain).astype(bf16)
    sh[1, z, pl.ds(yr64, 64), :] = (su_ref[...] * gain).astype(bf16)
    sh[2, z, pl.ds(yr64, 64), :] = sd_ref[...].astype(bf16)

    col = pl.multiple_of(tp * 128, 128)
    frow = pl.multiple_of(fs * 64, 64)

    def convert(m):
        def one(e, _):
            if m == 2:
                wsend[2, e] = ed_ref[e].astype(bf16)
            else:
                wsend[m, e] = ((eg_ref, eu_ref)[m][e] * gain).astype(bf16)
            return 0

        lax.fori_loop(0, 32, one, 0)
        w[m, pl.ds(frow, 64), pl.ds(col, 128)] = wsend[m, fs]

    convert(0)
    pl.semaphore_wait(barrier, 38)

    def a2a(m, lo, hi):
        def one(i, _):
            dz, dy = i // NY, i % NY
            peer = ((z + dz) % NZ) * NY + (y + dy) % NY
            rc(wsend.at[m, peer], w.at[m, pl.ds(frow, 64), pl.ds(col, 128)],
               send.at[A2A + m], recv.at[A2A + m], (peer, tp)).start()
            return 0

        lax.fori_loop(lo, hi, one, 0)

    def a2a_desc(m):
        return rc(wsend.at[m, pl.ds(0, 31)], wsend.at[m, pl.ds(0, 31)],
                  send.at[A2A + m], recv.at[A2A + m], (fs, tp))

    started = []

    def go(d):
        d.start()
        started.append(d)

    def tkz(zi, half=None):
        if half is None:
            return tk.at[zi, pl.ds(yrow, 32), :]
        return tk.at[zi, pl.ds(pl.multiple_of(yrow + 16 * half, 16), 16), :]

    def shz(zi, half=None):
        if half is None:
            return sh.at[:, zi]
        return sh.at[:, zi, pl.ds(128 * half, 128), :]

    def zring(k, view, base):
        br, bl = (z - k + 1 + NZ) % NZ, (z + k - 1) % NZ
        hr, hl = (None, None) if k < 4 else (0, 1)
        go(rc(view(br, hr), view(br, hr), send.at[base + k - 1], recv.at[base + k - 1], (at_z(1), tp)))
        go(rc(view(bl, hl), view(bl, hl), send.at[base + 3 + k], recv.at[base + 3 + k], (at_z(-1), tp)))

    def zwait(k, view, base):
        br, bl = (z - k + NZ) % NZ, (z + k) % NZ
        hr, hl = (None, None) if k < 4 else (0, 1)
        rc(view(br, hr), view(br, hr), send.at[base + k - 1], recv.at[base + k - 1], (fs, tp)).wait_recv()
        rc(view(bl, hl), view(bl, hl), send.at[base + 3 + k], recv.at[base + 3 + k], (fs, tp)).wait_recv()

    def tky(yi, lo=0, n=8):
        return tk.at[pl.ds(lo, n), pl.ds(pl.multiple_of(((yi + NY) % NY) * 32, 32), 32), :]

    def shy(yi, lo=0, n=8):
        return sh.at[:, z, pl.ds(pl.multiple_of(((yi + NY) % NY) * 64 + lo * 8, 32), n * 8), :]

    def yring(k, view, base):
        if k == 1:
            go(rc(view(y), view(y), send.at[base], recv.at[base], (at_y(1), tp)))
            go(rc(view(y), view(y), send.at[base + 1], recv.at[base + 1], (at_y(-1), tp)))
        else:
            go(rc(view(y - 1, 0, 4), view(y - 1, 0, 4), send.at[base + 2], recv.at[base + 2], (at_y(1), tp)))
            go(rc(view(y + 1, 4, 4), view(y + 1, 4, 4), send.at[base + 3], recv.at[base + 3], (at_y(-1), tp)))

    def ywait(k, view, base):
        if k == 1:
            rc(view(y - 1), view(y - 1), send.at[base], recv.at[base], (fs, tp)).wait_recv()
            rc(view(y + 1), view(y + 1), send.at[base + 1], recv.at[base + 1], (fs, tp)).wait_recv()
        else:
            rc(view(y - 2, 0, 4), view(y - 2, 0, 4), send.at[base + 2], recv.at[base + 2], (fs, tp)).wait_recv()
            rc(view(y + 2, 4, 4), view(y + 2, 4, 4), send.at[base + 3], recv.at[base + 3], (fs, tp)).wait_recv()

    def wcol(m, xi, ci, part=None):
        cc = pl.multiple_of((((xi + NX) % NX) * 2 + ci) * 128, 128)
        if part is None:
            return w.at[m, :, pl.ds(cc, 128)]
        return w.at[m, pl.ds(part * 1024, 1024), pl.ds(cc, 128)]

    def xs(m, j):
        return XAG + m * 9 + j

    def xsend(m, j, xi, part, dev):
        v = wcol(m, xi, c, part)
        go(rc(v, v, send.at[xs(m, j)], recv.at[xs(m, j)], (fs, dev)))

    def xwait(m, j, xi, ci, part):
        v = wcol(m, xi, ci, part)
        rc(v, v, send.at[xs(m, j)], recv.at[xs(m, j)], (fs, tp)).wait_recv()

    def x1(m):
        xsend(m, 0, x, None, xr)
        xsend(m, 1, x, None, xl)
        xsend(m, 4, x, None, mate)

    def x2(m):
        xwait(m, 0, x - 1, c, None)
        xsend(m, 2, x - 1, 0, xr)
        xsend(m, 5, x - 1, None, mate)
        xwait(m, 1, x + 1, c, None)
        xsend(m, 3, x + 1, 1, xl)
        xsend(m, 6, x + 1, None, mate)

    def x3(m):
        xwait(m, 2, x - 2, c, 0)
        xsend(m, 7, x - 2, 0, mate)
        xwait(m, 3, x + 2, c, 1)
        xsend(m, 8, x + 2, 1, mate)

    def x4(m):
        xwait(m, 4, x, 1 - c, None)
        xwait(m, 5, x - 1, 1 - c, None)
        xwait(m, 6, x + 1, 1 - c, None)
        xwait(m, 7, x - 2, 1 - c, 0)
        xwait(m, 8, x + 2, 1 - c, 1)


    def gate_up(m):
        def one(i, _):
            r, n = i // 4, i % 4
            lhs = tk[pl.ds(4 * r, 4), :, 0:2048].reshape(512, 2048)
            cs = pl.ds(pl.multiple_of(n * 256, 256), 256)
            acc = jnp.dot(lhs, w[m, :, cs], preferred_element_type=f32)
            rs = pl.ds(pl.multiple_of(r * 512, 512), 512)
            if m == 0:
                gbuf[rs, cs] = acc
            else:
                g = gbuf[rs, cs]
                hbuf[rs, cs] = (g / (1.0 + jnp.exp(-g)) * acc).astype(bf16)
            return 0

        lax.fori_loop(0, 8, one, 0)

    lanes = lax.broadcasted_iota(jnp.int32, (1, 128), 1)
    mine = (lanes % 32 == fs) & (lanes < 96)

    def down(half):
        def one(i, _):
            r, n = i // 4, i % 4
            cs = pl.ds(pl.multiple_of(half * 1024 + n * 256, 256), 256)
            rs = pl.ds(pl.multiple_of(r * 512, 512), 512)
            acc = lax.dot_general(hbuf[rs, :], w[2, cs, :], (((1,), (1,)), ((), ())), preferred_element_type=f32)
            wt = tk[pl.ds(4 * r, 4), :, 2048:2176].reshape(512, 128).astype(f32)
            scale = jnp.sum(jnp.where(mine, wt, 0.0), axis=1, keepdims=True)
            ob[pl.ds(4 * r, 4), :, cs] = (acc * scale).astype(bf16).reshape(4, 128, 256)
            return 0

        lax.fori_loop(0, 8, one, 0)

    def bf_add(dst, a, n):
        def one(i, _):
            rs = pl.ds(pl.multiple_of(i * 16, 16), 16)
            dst[rs, :] = (dst[rs, :].astype(f32) + a[rs, :].astype(f32)).astype(bf16)
            return 0

        lax.fori_loop(0, n, one, 0)

    CA, CB = pl.ds(0, 1024), pl.ds(1024, 1024)

    def az(k, s):
        d = (z + s * (5 - k) + NZ) % NZ
        if k == 1:
            return ob.at[d, pl.ds(0 if s == 1 else 64, 64), CA]
        return ob.at[d, :, CA]

    def az_slot(k, s):
        j = 0 if s == 1 else 1
        if k == 1:
            return ra.at[j, 0, pl.ds(0, 64), :]
        return ra.at[j, k - 1]

    def az_copy(k, s):
        q = RAZ + (0 if s == 1 else 4) + k - 1
        return rc(az(k, s), az_slot(k, s), send.at[q], recv.at[q], (at_z(s), tp))

    def az_go(k):
        go(az_copy(k, 1))
        go(az_copy(k, -1))

    def az_in(k):
        for s in (1, -1):
            az_copy(k, s).wait_recv()
            d = (z + s * (4 - k) + NZ) % NZ
            if k == 1:
                bf_add(ob.at[d, pl.ds(0 if s == 1 else 64, 64), CA], az_slot(1, s), 4)
            elif k < 4:
                bf_add(ob.at[d, :, CA], az_slot(k, s), 8)
        if k == 4:
            def one(i, _):
                rs = pl.ds(pl.multiple_of(i * 16, 16), 16)
                sa[rs, :] = (ob[z, rs, CA].astype(f32) + ra[0, 3, rs, :].astype(f32) + ra[1, 3, rs, :].astype(f32)).astype(bf16)
                return 0

            lax.fori_loop(0, 8, one, 0)

    def yrows(d, k, s):
        lo_ = ((d + NY) % NY) * 32
        if k == 1:
            return pl.ds(pl.multiple_of(lo_ + (0 if s == 1 else 16), 16), 16)
        return pl.ds(pl.multiple_of(lo_, 32), 32)

    def ay_copy(k, s):
        q = RAY + (0 if s == 1 else 2) + k - 1
        j = 0 if s == 1 else 1
        slot = ya.at[j, 0, pl.ds(0, 16), :] if k == 1 else ya.at[j, 1]
        return rc(sa.at[yrows(y + s * (3 - k), k, s), :], slot, send.at[q], recv.at[q], (at_y(s), tp))

    def ay_go(k):
        go(ay_copy(k, 1))
        go(ay_copy(k, -1))

    def ay_in1():
        for s in (1, -1):
            ay_copy(1, s).wait_recv()
            bf_add(sa.at[yrows(y + s, 1, s), :], ya.at[0 if s == 1 else 1, 0, pl.ds(0, 16), :], 1)

    def by_copy(k, s):
        q = RBY + (0 if s == 1 else 2) + k - 1
        j = 0 if s == 1 else 1
        slot = yb.at[j, 0, :, pl.ds(0, 16), :] if k == 1 else yb.at[j, 1]
        return rc(ob.at[:, yrows(y + s * (3 - k), k, s), CB], slot, send.at[q], recv.at[q], (at_y(s), tp))

    def by_go(k):
        go(by_copy(k, 1))
        go(by_copy(k, -1))

    def by_in(k):
        for s in (1, -1):
            by_copy(k, s).wait_recv()
        if k == 1:
            for s in (1, -1):
                def one(i, _):
                    rs = yrows(y + s, 1, s)
                    ob[i, rs, CB] = (ob[i, rs, CB].astype(f32) + yb[0 if s == 1 else 1, 0, i, 0:16, :].astype(f32)).astype(bf16)
                    return 0

                lax.fori_loop(0, 8, one, 0)
        else:
            def two(i, _):
                rs = yrows(y, 2, 1)
                ob[i, rs, CB] = (ob[i, rs, CB].astype(f32) + yb[0, 1, i].astype(f32) + yb[1, 1, i].astype(f32)).astype(bf16)
                return 0

            lax.fori_loop(0, 8, two, 0)

    def bz_rows(k, s):
        if k == 1:
            return pl.ds(pl.multiple_of(yrow + (0 if s == 1 else 16), 16), 16)
        return pl.ds(yrow, 32)

    def bz_slot(k, s):
        j = 0 if s == 1 else 1
        return zb.at[j, 0, pl.ds(0, 16), :] if k == 1 else zb.at[j, k - 1]

    def bz_copy(k, s):
        q = RBZ + (0 if s == 1 else 4) + k - 1
        d = (z + s * (5 - k) + NZ) % NZ
        return rc(ob.at[d, bz_rows(k, s), CB], bz_slot(k, s), send.at[q], recv.at[q], (at_z(s), tp))

    def bz_go(k):
        go(bz_copy(k, 1))
        go(bz_copy(k, -1))

    def bz_in(k):
        for s in (1, -1):
            bz_copy(k, s).wait_recv()
            d = (z + s * (4 - k) + NZ) % NZ
            if k < 4:
                bf_add(ob.at[d, bz_rows(k, s), CB], bz_slot(k, s), 1 if k == 1 else 2)

    def shared():
        cg = sh[0].reshape(2048, 128)
        cu = sh[1].reshape(2048, 128)
        nrm = nb[...]
        g = jnp.dot(nrm, cg, preferred_element_type=f32)
        u = jnp.dot(nrm, cu, preferred_element_type=f32)
        h = (g / (1.0 + jnp.exp(-g)) * u).astype(bf16)

        def one(i, _):
            cd = sh[2, i]
            cs = pl.ds(pl.multiple_of(i * 256, 256), 256)
            sp[:, cs] = lax.dot_general(h, cd, (((1,), (1,)), ((), ())), preferred_element_type=f32).astype(bf16)
            return 0

        lax.fori_loop(0, 8, one, 0)
        trow = pl.ds(pl.multiple_of(tp * 32, 32), 32)

        def give(i, _):
            to = (tp + i) % 8
            rc(sp.at[pl.ds(pl.multiple_of(to * 32, 32), 32), :], sr.at[tp], send.at[SPX], recv.at[SPX], (fs, to)).start()
            return 0

        lax.fori_loop(1, 8, give, 0)
        sr[tp] = sp[trow, :]

    def spx_all():
        return rc(sr.at[pl.ds(0, 7)], sr.at[pl.ds(0, 7)], send.at[SPX], recv.at[SPX], (fs, tp))

    def normalize_all(i, _):
        rs = pl.ds(pl.multiple_of(i * 32, 32), 32)
        v = tok_ref[rs, :].astype(f32)
        nb[rs, :] = (v * lax.rsqrt(jnp.mean(v * v, axis=-1, keepdims=True) + 1e-6)).astype(bf16)
        return 0

    a2a(0, 1, 32)
    zring(1, tkz, TOKZ)
    convert(1)
    convert(2)
    a2a_desc(0).wait_recv()
    x1(0)
    zwait(1, tkz, TOKZ)
    zring(2, tkz, TOKZ)
    a2a(1, 1, 8)
    zwait(2, tkz, TOKZ)
    zring(3, tkz, TOKZ)
    a2a(1, 8, 16)
    zwait(3, tkz, TOKZ)
    zring(4, tkz, TOKZ)
    a2a(1, 16, 24)
    zwait(4, tkz, TOKZ)
    yring(1, tky, TOKY)
    a2a(1, 24, 32)
    yring(1, shy, SHY)
    lax.fori_loop(0, 8, normalize_all, 0)
    x2(0)
    a2a_desc(1).wait_recv()
    x1(1)
    a2a(2, 1, 32)
    ywait(1, shy, SHY)
    yring(2, shy, SHY)
    x3(0)
    a2a_desc(2).wait_recv()
    x1(2)
    ywait(2, shy, SHY)
    zring(1, shz, SHZ)
    x2(1)
    zwait(1, shz, SHZ)
    zring(2, shz, SHZ)
    ywait(1, tky, TOKY)
    yring(2, tky, TOKY)
    x3(1)
    zwait(2, shz, SHZ)
    zring(3, shz, SHZ)
    x4(0)
    zwait(3, shz, SHZ)
    zring(4, shz, SHZ)
    ywait(2, tky, TOKY)
    outs = [
        pltpu.make_async_copy(w.at[0, :, pl.ds(col, 128)], sg_out, loc.at[0]),
        pltpu.make_async_copy(w.at[1, :, pl.ds(col, 128)], su_out, loc.at[1]),
        pltpu.make_async_copy(w.at[2, :, pl.ds(col, 128)], sd_out, loc.at[2]),
    ]
    for o in outs:
        o.start()
    gate_up(0)
    x2(2)
    x4(1)
    gate_up(1)
    x3(2)
    zwait(4, shz, SHZ)
    cm = pltpu.make_async_copy(sh, cm_out, loc.at[3])
    cm.start()
    x4(2)
    down(0)
    az_go(1)
    down(1)
    by_go(1)
    shared()
    az_in(1)
    az_go(2)
    by_in(1)
    by_go(2)
    az_in(2)
    az_go(3)
    az_in(3)
    az_go(4)
    by_in(2)
    bz_go(1)
    bz_in(1)
    bz_go(2)
    az_in(4)
    ay_go(1)
    bz_in(2)
    bz_go(3)
    ay_in1()
    ay_go(2)
    bz_in(3)
    bz_go(4)
    spx_all().wait_recv()
    for s in (1, -1):
        ay_copy(2, s).wait_recv()
    bz_in(4)

    def finish(i, _):
        rs = pl.ds(pl.multiple_of(i * 16, 16), 16)
        rs_y = pl.ds(pl.multiple_of(yrow + i * 16, 16), 16)
        a = sa[rs_y, :].astype(f32) + ya[0, 1, rs, :].astype(f32) + ya[1, 1, rs, :].astype(f32)
        b = ob[z, rs_y, CB].astype(f32) + zb[0, 3, rs, :].astype(f32) + zb[1, 3, rs, :].astype(f32)
        for q in range(8):
            a = a + sr[q, rs, 0:1024].astype(f32)
            b = b + sr[q, rs, 1024:2048].astype(f32)
        for q in range(4):
            fin[q, rs, :] = a[:, q * 256 : q * 256 + 256].astype(bf16)
            fin[4 + q, rs, :] = b[:, q * 256 : q * 256 + 256].astype(bf16)
        return 0

    lax.fori_loop(0, 2, finish, 0)

    def give(i, _):
        to = (tp + i) % 8
        rc(fin.at[to], lo.at[tp], send.at[FIN], recv.at[FIN], (fs, to)).start()
        return 0

    lax.fori_loop(1, 8, give, 0)
    lo[tp] = fin[tp]
    fin_all = rc(fin.at[pl.ds(0, 7)], lo.at[pl.ds(0, 7)], send.at[FIN], recv.at[FIN], (fs, tp))
    for m in range(3):
        a2a_desc(m).wait_send()
    for d in started:
        d.wait_send()
    spx_all().wait_send()
    for o in outs:
        o.wait()
    cm.wait()
    fin_all.wait_recv()
    last = pltpu.make_async_copy(lo, lo_out, loc.at[4])
    last.start()
    fin_all.wait_send()
    last.wait()


def fused(tokens, dense3, gain, eg, eu, ed, sg, su, sd):
    any_ = pl.BlockSpec(memory_space=pl.ANY)
    vm = pl.BlockSpec(memory_space=pltpu.VMEM)
    V = pltpu.VMEM
    return pl.pallas_call(
        kernel,
        out_shape=[jax.ShapeDtypeStruct((8, 32, 256), bf16)]
        + [jax.ShapeDtypeStruct((2048, 128), bf16)] * 3
        + [jax.ShapeDtypeStruct((3, 8, 256, 128), bf16)],
        in_specs=[vm] * 9,
        out_specs=[any_] * 5,
        scratch_shapes=[
            V((3, 32, 64, 128), bf16),
            V((3, 2048, 1024), bf16),
            V((8, 128, COLS), bf16),
            V((3, 8, 256, 128), bf16),
            V((256, 2048), bf16),
            V((1024, 1024), f32),
            V((1024, 1024), bf16),
            V((8, 128, 2048), bf16),
            V((2, 4, 128, 1024), bf16),
            V((2, 2, 32, 1024), bf16),
            V((2, 2, 8, 32, 1024), bf16),
            V((2, 4, 32, 1024), bf16),
            V((128, 1024), bf16),
            V((256, 2048), bf16),
            V((8, 32, 2048), bf16),
            V((8, 32, 256), bf16),
            V((8, 32, 256), bf16),
            pltpu.SemaphoreType.DMA((NSEM,)),
            pltpu.SemaphoreType.DMA((NSEM,)),
            pltpu.SemaphoreType.DMA((5,)),
        ],
        compiler_params=pltpu.CompilerParams(collective_id=0, has_side_effects=True, vmem_limit_bytes=60 * 2**20),
    )(tokens, dense3, gain, eg, eu, ed, sg, su, sd)


def body(tokens, routes, route_weights, norm_gain, expert_gate, expert_up, expert_down, shared_gate, shared_up, shared_down):
    experts = jnp.arange(32, dtype=jnp.int32)
    hits = routes[:, :, None] == experts[None, None, :]
    dense = jnp.sum(jnp.where(hits, route_weights[:, :, None], 0.0), axis=1)
    high = lax.reduce_precision(dense, 8, 7)
    mid = lax.reduce_precision(dense - high, 8, 7)
    low = dense - high - mid
    dense3 = jnp.concatenate([high, mid, low, jnp.zeros_like(low)], axis=1).astype(bf16)
    gain = jnp.broadcast_to(norm_gain[:, None], (64, 128))
    lo, sg, su, sd, cm = fused(tokens, dense3, gain, expert_gate, expert_up, expert_down, shared_gate, shared_up, shared_down)
    cm = cm.reshape(3, 2048, 128)
    return lo.reshape(256, 256), sg[None], su[None], sd[None], cm[0], cm[1], cm[2]


def solution(mesh):
    return jax.shard_map(
        body,
        mesh=mesh,
        in_specs=(P("fs", None), P("fs", None), P("fs", None), P("fs"), P(None, "fs", "tp"), P(None, "fs", "tp"), P(None, "fs", "tp"), P("fs", "tp"), P("fs", "tp"), P("fs", "tp")),
        out_specs=(P("fs", "tp"), P("fs", None, "tp"), P("fs", None, "tp"), P("fs", None, "tp"), P(None, "tp"), P(None, "tp"), P(None, "tp")),
        check_vma=False,
    )
```

```python
import functools
import jax
import jax.numpy as jnp
from jax import lax
from jax.experimental import pallas as pl
from jax.experimental.pallas import tpu as pltpu
from jax.sharding import PartitionSpec as P

MESH = pl.DeviceIdType.MESH
bf16, f32 = jnp.bfloat16, jnp.float32
NZ, NY, NX = 8, 4, 4
COLS = 2048 + 128

A2A = 0
TOKZ = 6
TOKY = 14
SHZ = 38
SHY = 46
XAG = 50
RAZ = 104
RAY = 120
RBY = 128
RBZ = 136
SPX = 152
FIN = 153
NSEM = 154


def rc(src, dst, ssem, rsem, dev):
    return pltpu.make_async_remote_copy(
        src_ref=src, dst_ref=dst, send_sem=ssem, recv_sem=rsem, device_id=dev, device_id_type=MESH
    )


def kernel(
    tok_hbm, rt_hbm, rw_hbm, gn_hbm, eg_hbm, eu_hbm, ed_hbm, sg_hbm, su_hbm, sd_hbm,
    lo_out, sg_out, su_out, sd_out, cg_out, cu_out, cd_out,
    tok_ref, rt_ref, rw_ref, gn_ref, ew_ref, sw_ref,
    wsend, w, tk, sh, nb, gbuf, hbuf, ob, ra, ya, yb, zb, sa, sp, sr, fin, lo, send, recv, loc,
):
    fs, tp = lax.axis_index("fs"), lax.axis_index("tp")
    z, y = fs // NY, fs % NY
    x, c = tp // 2, tp % 2

    def at_z(d):
        return ((z + d + NZ) % NZ) * NY + y

    def at_y(d):
        return z * NY + (y + d + NY) % NY

    xr, xl = ((x + 1) % NX) * 2 + c, ((x + NX - 1) % NX) * 2 + c
    mate = x * 2 + 1 - c

    barrier = pltpu.get_barrier_semaphore()

    def sig_fs(i, _):
        pl.semaphore_signal(barrier, inc=1, device_id=((fs + i) % 32, tp), device_id_type=MESH)
        return 0

    def sig_tp(i, _):
        pl.semaphore_signal(barrier, inc=1, device_id=(fs, (tp + i) % 8), device_id_type=MESH)
        return 0

    fetch = [
        pltpu.make_async_copy(a, b, loc.at[n])
        for n, (a, b) in enumerate(
            [
                (gn_hbm, gn_ref), (eg_hbm, ew_ref.at[0]), (tok_hbm, tok_ref), (rt_hbm, rt_ref), (rw_hbm, rw_ref),
                (sg_hbm, sw_ref.at[0]), (su_hbm, sw_ref.at[1]), (sd_hbm, sw_ref.at[2]),
                (eu_hbm, ew_ref.at[1]), (ed_hbm, ew_ref.at[2]),
            ]
        )
    ]
    for f in fetch:
        f.start()
    lax.fori_loop(1, 32, sig_fs, 0)
    lax.fori_loop(1, 8, sig_tp, 0)

    yrow = pl.multiple_of(y * 32, 32)
    yr64 = pl.multiple_of(y * 64, 64)
    col = pl.multiple_of(tp * 128, 128)
    srow = pl.ds(pl.multiple_of(tp * 32, 32), 32)

    fetch[0].wait()
    eye = lax.broadcasted_iota(jnp.int32, (64, 64), 0) == lax.broadcasted_iota(jnp.int32, (64, 64), 1)
    gain = jnp.sum(jnp.where(eye, gn_ref[...], 0.0), axis=1, keepdims=True)

    def convert(m):
        def one(e, _):
            if m == 2:
                wsend[2, e] = ew_ref[2, e].astype(bf16)
            else:
                wsend[m, e] = (ew_ref[m, e] * gain).astype(bf16)
            return 0

        lax.fori_loop(0, 32, one, 0)
        w[m, fs, :, pl.ds(col, 128)] = wsend[m, fs]

    fetch[1].wait()
    convert(0)

    for n in (2, 3, 4):
        fetch[n].wait()
    rows = tok_ref[srow, :].astype(f32)
    scale = lax.rsqrt(jnp.mean(rows * rows, axis=-1, keepdims=True) + 1e-6)
    tk[z, pl.ds(yrow, 32), 0:2048] = (rows * scale).astype(bf16)
    lanes = lax.broadcasted_iota(jnp.int32, (1, 128), 1)
    expert = lax.broadcasted_iota(jnp.int32, (128, 1), 0)
    dense = jnp.zeros((128, 256), f32)
    for k in range(6):
        dense = dense + jnp.where(rt_ref[k : k + 1, :] == expert % 32, rw_ref[k : k + 1, :], 0.0)
    high = dense.astype(bf16).astype(f32)
    mid = (dense - high).astype(bf16).astype(f32)
    low = dense - high - mid
    terms = jnp.where(expert < 32, high, jnp.where(expert < 64, mid, jnp.where(expert < 96, low, 0.0)))
    pick = lax.broadcasted_iota(jnp.int32, (32, 256), 1) == lax.broadcasted_iota(jnp.int32, (32, 256), 0) + tp * 32
    tk[z, pl.ds(yrow, 32), 2048:2176] = lax.dot_general(
        jnp.where(pick, 1.0, 0.0).astype(bf16), terms.astype(bf16), (((1,), (1,)), ((), ())), preferred_element_type=f32
    ).astype(bf16)
    for n in (5, 6, 7):
        fetch[n].wait()
    sh[0, z, pl.ds(yr64, 64), :] = (sw_ref[0] * gain).astype(bf16)
    sh[1, z, pl.ds(yr64, 64), :] = (sw_ref[1] * gain).astype(bf16)
    sh[2, z, pl.ds(yr64, 64), :] = sw_ref[2].astype(bf16)
    pl.semaphore_wait(barrier, 38)

    def a2a(j):
        m, h = j // 2, pl.ds(32 * (j % 2), 32)

        def one(i, _):
            dz, dy = i // NY, i % NY
            peer = ((z + dz) % NZ) * NY + (y + dy) % NY
            rc(wsend.at[m, peer, h], w.at[m, fs, h, pl.ds(col, 128)],
               send.at[A2A + j], recv.at[A2A + j], (peer, tp)).start()
            return 0

        lax.fori_loop(1, 32, one, 0)

    def a2a_desc(j):
        v = wsend.at[j // 2, pl.ds(0, 31), pl.ds(32 * (j % 2), 32)]
        return rc(v, v, send.at[A2A + j], recv.at[A2A + j], (fs, tp))

    started = []

    def go(d):
        d.start()
        started.append(d)

    def tkz(zi, half=None):
        if half is None:
            return tk.at[zi, pl.ds(yrow, 32), :]
        return tk.at[zi, pl.ds(pl.multiple_of(yrow + 16 * half, 16), 16), :]

    def shz(zi, half=None):
        if half is None:
            return sh.at[:, zi]
        return sh.at[:, zi, pl.ds(128 * half, 128), :]

    def zring(k, view, base):
        br, bl = (z - k + 1 + NZ) % NZ, (z + k - 1) % NZ
        hr, hl = (None, None) if k < 4 else (0, 1)
        go(rc(view(br, hr), view(br, hr), send.at[base + k - 1], recv.at[base + k - 1], (at_z(1), tp)))
        go(rc(view(bl, hl), view(bl, hl), send.at[base + 3 + k], recv.at[base + 3 + k], (at_z(-1), tp)))

    def zwait(k, view, base):
        br, bl = (z - k + NZ) % NZ, (z + k) % NZ
        hr, hl = (None, None) if k < 4 else (0, 1)
        rc(view(br, hr), view(br, hr), send.at[base + k - 1], recv.at[base + k - 1], (fs, tp)).wait_recv()
        rc(view(bl, hl), view(bl, hl), send.at[base + 3 + k], recv.at[base + 3 + k], (fs, tp)).wait_recv()

    def tkb(o, yi):
        return tk.at[(z + o) % NZ, pl.ds(pl.multiple_of(((yi + NY) % NY) * 32, 32), 32), :]

    def ty1(*offsets):
        for o in offsets:
            go(rc(tkb(o, y), tkb(o, y), send.at[TOKY + o], recv.at[TOKY + o], (at_y(1), tp)))
            go(rc(tkb(o, y), tkb(o, y), send.at[TOKY + 8 + o], recv.at[TOKY + 8 + o], (at_y(-1), tp)))

    def ty_wait(n, o, yi):
        rc(tkb(o, yi), tkb(o, yi), send.at[n], recv.at[n], (fs, tp)).wait_recv()

    def ty2(*offsets):
        for o in offsets:
            s = 1 if o < 4 else -1
            ty_wait(TOKY + (0 if o < 4 else 8) + o, o, y - s)
            go(rc(tkb(o, y - s), tkb(o, y - s), send.at[TOKY + 16 + o], recv.at[TOKY + 16 + o], (at_y(s), tp)))

    def ty_in1():
        for o in range(8):
            s = 1 if o < 4 else -1
            ty_wait(TOKY + (8 if o < 4 else 0) + o, o, y + s)

    def ty_in2():
        for o in range(8):
            ty_wait(TOKY + 16 + o, o, y + 2)

    def shy(yi, lo=0, n=8):
        return sh.at[:, z, pl.ds(pl.multiple_of(((yi + NY) % NY) * 64 + lo * 8, 32), n * 8), :]

    def yring(k, view, base):
        if k == 1:
            go(rc(view(y), view(y), send.at[base], recv.at[base], (at_y(1), tp)))
            go(rc(view(y), view(y), send.at[base + 1], recv.at[base + 1], (at_y(-1), tp)))
        else:
            go(rc(view(y - 1, 0, 4), view(y - 1, 0, 4), send.at[base + 2], recv.at[base + 2], (at_y(1), tp)))
            go(rc(view(y + 1, 4, 4), view(y + 1, 4, 4), send.at[base + 3], recv.at[base + 3], (at_y(-1), tp)))

    def ywait(k, view, base):
        if k == 1:
            rc(view(y - 1), view(y - 1), send.at[base], recv.at[base], (fs, tp)).wait_recv()
            rc(view(y + 1), view(y + 1), send.at[base + 1], recv.at[base + 1], (fs, tp)).wait_recv()
        else:
            rc(view(y - 2, 0, 4), view(y - 2, 0, 4), send.at[base + 2], recv.at[base + 2], (fs, tp)).wait_recv()
            rc(view(y + 2, 4, 4), view(y + 2, 4, 4), send.at[base + 3], recv.at[base + 3], (fs, tp)).wait_recv()

    def wcol(j, xi, ci, part=None):
        cc = pl.multiple_of((((xi + NX) % NX) * 2 + ci) * 128, 128)
        m, h = j // 2, pl.ds(32 * (j % 2), 32)
        if part is None:
            return w.at[m, :, h, pl.ds(cc, 128)]
        return w.at[m, pl.ds(part * 16, 16), h, pl.ds(cc, 128)]

    def xs(m, j):
        return XAG + m * 9 + j

    def xsend(m, j, xi, part, dev):
        v = wcol(m, xi, c, part)
        go(rc(v, v, send.at[xs(m, j)], recv.at[xs(m, j)], (fs, dev)))

    def xwait(m, j, xi, ci, part):
        v = wcol(m, xi, ci, part)
        rc(v, v, send.at[xs(m, j)], recv.at[xs(m, j)], (fs, tp)).wait_recv()

    def x1(m):
        xsend(m, 0, x, None, xr)
        xsend(m, 1, x, None, xl)
        xsend(m, 4, x, None, mate)

    def x2(m):
        xwait(m, 0, x - 1, c, None)
        xsend(m, 2, x - 1, 0, xr)
        xsend(m, 5, x - 1, None, mate)
        xwait(m, 1, x + 1, c, None)
        xsend(m, 3, x + 1, 1, xl)
        xsend(m, 6, x + 1, None, mate)

    def x3(m):
        xwait(m, 2, x - 2, c, 0)
        xsend(m, 7, x - 2, 0, mate)
        xwait(m, 3, x + 2, c, 1)
        xsend(m, 8, x + 2, 1, mate)

    def x4(m):
        xwait(m, 4, x, 1 - c, None)
        xwait(m, 5, x - 1, 1 - c, None)
        xwait(m, 6, x + 1, 1 - c, None)
        xwait(m, 7, x - 2, 1 - c, 0)
        xwait(m, 8, x + 2, 1 - c, 1)


    def gate_up(m, dy):
        rs = pl.ds(pl.multiple_of(((y + dy + NY) % NY) * 32, 32), 32)

        def one(n, _):
            lhs = tk[:, rs, 0:2048].reshape(256, 2048)
            cs = pl.ds(pl.multiple_of(n * 512, 512), 512)
            acc = jnp.dot(lhs, w[m, :, :, cs].reshape(2048, 512), preferred_element_type=f32)
            acc = acc.reshape(8, 32, 512)
            if m == 0:
                gbuf[:, rs, cs] = acc
            else:
                g = gbuf[:, rs, cs]
                hbuf[:, rs, cs] = (g / (1.0 + jnp.exp(-g)) * acc).astype(bf16)
            return 0

        lax.fori_loop(0, 2, one, 0)

    mine = (lanes % 32 == fs) & (lanes < 96)

    def down(quarter):
        def one(r, _):
            cs = pl.ds(quarter * 512, 512)
            wd = w[2, pl.ds(quarter * 8, 8)].reshape(512, 1024)
            h = hbuf[pl.ds(4 * r, 4)].reshape(512, 1024)
            acc = lax.dot_general(h, wd, (((1,), (1,)), ((), ())), preferred_element_type=f32)
            wt = tk[pl.ds(4 * r, 4), :, 2048:2176].reshape(512, 128).astype(f32)
            scale = jnp.sum(jnp.where(mine, wt, 0.0), axis=1, keepdims=True)
            ob[pl.ds(4 * r, 4), :, cs] = (acc * scale).astype(bf16).reshape(4, 128, 512)
            return 0

        lax.fori_loop(0, 2, one, 0)

    def bf_add(dst, a, n):
        def one(i, _):
            rs = pl.ds(pl.multiple_of(i * 16, 16), 16)
            dst[rs, :] = (dst[rs, :].astype(f32) + a[rs, :].astype(f32)).astype(bf16)
            return 0

        lax.fori_loop(0, n, one, 0)

    def ca(q):
        return pl.ds(q * 512, 512)

    def cb(q):
        return pl.ds(1024 + q * 512, 512)

    def az(q, k, s):
        d = (z + s * (5 - k) + NZ) % NZ
        if k == 1:
            return ob.at[d, pl.ds(0 if s == 1 else 64, 64), ca(q)]
        return ob.at[d, :, ca(q)]

    def az_slot(q, k, s):
        j = 0 if s == 1 else 1
        if k == 1:
            return ra.at[j, 0, pl.ds(0, 64), ca(q)]
        return ra.at[j, k - 1, :, ca(q)]

    def az_copy(q, k, s):
        n = RAZ + 8 * q + (0 if s == 1 else 4) + k - 1
        return rc(az(q, k, s), az_slot(q, k, s), send.at[n], recv.at[n], (at_z(s), tp))

    def az_go(q, k):
        go(az_copy(q, k, 1))
        go(az_copy(q, k, -1))

    def az_in(q, k):
        for s in (1, -1):
            az_copy(q, k, s).wait_recv()
            d = (z + s * (4 - k) + NZ) % NZ
            if k == 1:
                bf_add(ob.at[d, pl.ds(0 if s == 1 else 64, 64), ca(q)], az_slot(q, 1, s), 4)
            elif k < 4:
                bf_add(ob.at[d, :, ca(q)], az_slot(q, k, s), 8)
        if k == 4:
            def one(i, _):
                rs = pl.ds(pl.multiple_of(i * 16, 16), 16)
                c_ = ca(q)
                sa[rs, c_] = (ob[z, rs, c_].astype(f32) + ra[0, 3, rs, c_].astype(f32) + ra[1, 3, rs, c_].astype(f32)).astype(bf16)
                return 0

            lax.fori_loop(0, 8, one, 0)

    def yrows(d, k, s):
        lo_ = ((d + NY) % NY) * 32
        if k == 1:
            return pl.ds(pl.multiple_of(lo_ + (0 if s == 1 else 16), 16), 16)
        return pl.ds(pl.multiple_of(lo_, 32), 32)

    def ay_copy(q, d):
        n = RAY + 4 * q + d
        src = sa.at[pl.ds(pl.multiple_of(((y + d) % NY) * 32, 32), 32), ca(q)]
        return rc(src, ya.at[d - 1, :, ca(q)], send.at[n], recv.at[n], (at_y(d), tp))

    def ay_go(q):
        for d in (2, 1, 3):
            go(ay_copy(q, d))

    def ay_in(q):
        for d in (1, 2, 3):
            ay_copy(q, d).wait_recv()

    def by_slot(q, k, s):
        j = 0 if s == 1 else 1
        return yb.at[j, 0, :, pl.ds(0, 16), ca(q)] if k == 1 else yb.at[j, 1, :, :, ca(q)]

    def by_copy(q, k, s):
        n = RBY + 4 * q + (0 if s == 1 else 2) + k - 1
        return rc(ob.at[:, yrows(y + s * (3 - k), k, s), cb(q)], by_slot(q, k, s), send.at[n], recv.at[n], (at_y(s), tp))

    def by_go(q, k):
        go(by_copy(q, k, 1))
        go(by_copy(q, k, -1))

    def by_in(q, k):
        for s in (1, -1):
            by_copy(q, k, s).wait_recv()
            if k == 1:
                rs, j = yrows(y + s, 1, s), 0 if s == 1 else 1

                def one(i, _):
                    ob[i, rs, cb(q)] = (ob[i, rs, cb(q)].astype(f32) + yb[j, 0, i, 0:16, ca(q)].astype(f32)).astype(bf16)
                    return 0

                lax.fori_loop(0, 8, one, 0)
        if k == 2:
            rs2 = yrows(y, 2, 1)

            def two(i, _):
                ob[i, rs2, cb(q)] = (ob[i, rs2, cb(q)].astype(f32) + yb[0, 1, i, :, ca(q)].astype(f32) + yb[1, 1, i, :, ca(q)].astype(f32)).astype(bf16)
                return 0

            lax.fori_loop(0, 8, two, 0)

    def bz_copy(q, part, s):
        j = 0 if s == 1 else 1
        n = RBZ + 8 * q + 4 * j + part
        d = (z + s * (4 - part) + NZ) % NZ
        rows = pl.ds(yrow, 32)
        slot = zb.at[j, part, :, ca(q)]
        if part == 0:
            rows = pl.ds(pl.multiple_of(yrow + 16 * j, 16), 16)
            slot = zb.at[j, 0, pl.ds(0, 16), ca(q)]
        to = at_z(s) if part == 3 else at_z(2 * s)
        return rc(ob.at[d, rows, cb(q)], slot, send.at[n], recv.at[n], (to, tp))

    def bz_go(q, *parts):
        for part in parts:
            go(bz_copy(q, part, 1))
            go(bz_copy(q, part, -1))

    def bz_in1(q):
        for s in (1, -1):
            j = 0 if s == 1 else 1
            bz_copy(q, 1, s).wait_recv()
            bf_add(ob.at[(z + s + NZ) % NZ, pl.ds(yrow, 32), cb(q)], zb.at[j, 1, :, ca(q)], 2)
        bz_go(q, 3)
        for s in (1, -1):
            j = 0 if s == 1 else 1
            bz_copy(q, 0, s).wait_recv()
            half = pl.ds(pl.multiple_of(yrow + 16 * j, 16), 16)
            bf_add(ob.at[(z + 2 * s + NZ) % NZ, half, cb(q)], zb.at[j, 0, pl.ds(0, 16), ca(q)], 1)
        bz_go(q, 2)

    def bz_in2(q):
        for part in (2, 3):
            for s in (1, -1):
                bz_copy(q, part, s).wait_recv()

    def shared():
        cg = sh[0].reshape(2048, 128)
        cu = sh[1].reshape(2048, 128)
        nrm = nb[...]
        g = jnp.dot(nrm, cg, preferred_element_type=f32)
        u = jnp.dot(nrm, cu, preferred_element_type=f32)
        h = (g / (1.0 + jnp.exp(-g)) * u).astype(bf16)

        def one(i, _):
            cd = sh[2, i]
            cs = pl.ds(pl.multiple_of(i * 256, 256), 256)
            sp[:, cs] = lax.dot_general(h, cd, (((1,), (1,)), ((), ())), preferred_element_type=f32).astype(bf16)
            return 0

        lax.fori_loop(0, 8, one, 0)
        trow = pl.ds(pl.multiple_of(tp * 32, 32), 32)

        def give(i, _):
            to = (tp + i) % 8
            rc(sp.at[pl.ds(pl.multiple_of(to * 32, 32), 32), :], sr.at[tp], send.at[SPX], recv.at[SPX], (fs, to)).start()
            return 0

        lax.fori_loop(1, 8, give, 0)
        sr[tp] = sp[trow, :]

    def spx_all():
        return rc(sr.at[pl.ds(0, 7)], sr.at[pl.ds(0, 7)], send.at[SPX], recv.at[SPX], (fs, tp))

    def normalize_all(i, _):
        rs = pl.ds(pl.multiple_of(i * 32, 32), 32)
        v = tok_ref[rs, :].astype(f32)
        nb[rs, :] = (v * lax.rsqrt(jnp.mean(v * v, axis=-1, keepdims=True) + 1e-6)).astype(bf16)
        return 0

    a2a(0)
    zring(1, tkz, TOKZ)
    ty1(0)
    yring(1, shy, SHY)
    fetch[8].wait()
    convert(1)
    fetch[9].wait()
    convert(2)
    a2a(1)
    zwait(1, tkz, TOKZ)
    zring(2, tkz, TOKZ)
    a2a(2)
    ty1(1, 7)
    a2a_desc(0).wait_recv()
    x1(0)
    a2a_desc(1).wait_recv()
    x1(1)
    zwait(2, tkz, TOKZ)
    zring(3, tkz, TOKZ)
    a2a(3)
    ty1(2, 6)
    x2(0)
    a2a_desc(2).wait_recv()
    x1(2)
    x2(1)
    zwait(3, tkz, TOKZ)
    zring(4, tkz, TOKZ)
    a2a(4)
    ty1(3, 5)
    x3(0)
    a2a_desc(3).wait_recv()
    x1(3)
    zwait(4, tkz, TOKZ)
    a2a(5)
    ty1(4)
    ty2(0)
    ywait(1, shy, SHY)
    yring(2, shy, SHY)
    x2(2)
    x3(1)
    ty2(1, 7)
    lax.fori_loop(0, 8, normalize_all, 0)
    a2a_desc(4).wait_recv()
    x1(4)
    ty2(2, 6)
    x2(3)
    x3(2)
    ty2(3, 5)
    ywait(2, shy, SHY)
    a2a_desc(5).wait_recv()
    x1(5)
    ty2(4)
    zring(1, shz, SHZ)
    ty_in1()
    x4(0)
    x4(1)
    gate_up(0, 0)
    x2(4)
    gate_up(0, 1)
    x3(3)
    gate_up(0, -1)
    zwait(1, shz, SHZ)
    zring(2, shz, SHZ)
    x2(5)
    x4(2)
    x4(3)
    gate_up(1, 0)
    x3(4)
    gate_up(1, 1)
    gate_up(1, -1)
    x3(5)
    zwait(2, shz, SHZ)
    zring(3, shz, SHZ)
    ty_in2()
    gate_up(0, 2)
    gate_up(1, 2)
    outs = [
        pltpu.make_async_copy(w.at[m, :, :, pl.ds(col, 128)], (sg_out, su_out, sd_out)[m], loc.at[m]) for m in range(3)
    ]
    commons = [pltpu.make_async_copy(sh.at[m], (cg_out, cu_out, cd_out)[m], loc.at[3 + m]) for m in range(3)]
    for o in outs:
        o.start()
    zwait(3, shz, SHZ)
    zring(4, shz, SHZ)
    x4(4)
    x4(5)
    down(2)
    by_go(0, 1)
    down(0)
    az_go(0, 1)
    down(3)
    by_go(1, 1)
    down(1)
    az_go(1, 1)
    by_in(0, 1)
    by_go(0, 2)
    az_in(0, 1)
    az_go(0, 2)
    by_in(1, 1)
    by_go(1, 2)
    az_in(1, 1)
    az_go(1, 2)
    zwait(4, shz, SHZ)
    shared()
    az_in(0, 2)
    az_go(0, 3)
    az_in(1, 2)
    az_go(1, 3)
    by_in(0, 2)
    bz_go(0, 1, 0)
    az_in(0, 3)
    az_go(0, 4)
    az_in(1, 3)
    az_go(1, 4)
    by_in(1, 2)
    bz_go(1, 1, 0)
    bz_in1(0)
    az_in(0, 4)
    ay_go(0)
    bz_in1(1)
    az_in(1, 4)
    ay_go(1)
    for m in range(3):
        commons[m].start()
    spx_all().wait_recv()
    ay_in(0)
    bz_in2(0)
    bz_in2(1)
    ay_in(1)

    def finish(i, _):
        rs = pl.ds(pl.multiple_of(i * 16, 16), 16)
        rs_y = pl.ds(pl.multiple_of(yrow + i * 16, 16), 16)
        a = sa[rs_y, :].astype(f32) + ya[0, rs, :].astype(f32) + ya[1, rs, :].astype(f32) + ya[2, rs, :].astype(f32)
        b = ob[z, rs_y, 1024:2048].astype(f32)
        for j in range(2):
            b = b + zb[j, 2, rs, :].astype(f32) + zb[j, 3, rs, :].astype(f32)
        for q in range(8):
            a = a + sr[q, rs, 0:1024].astype(f32)
            b = b + sr[q, rs, 1024:2048].astype(f32)
        for q in range(4):
            fin[q, rs, :] = a[:, q * 256 : q * 256 + 256].astype(bf16)
            fin[4 + q, rs, :] = b[:, q * 256 : q * 256 + 256].astype(bf16)
        return 0

    lax.fori_loop(0, 2, finish, 0)

    def give(i, _):
        to = (tp + i) % 8
        rc(fin.at[to], lo.at[tp], send.at[FIN], recv.at[FIN], (fs, to)).start()
        return 0

    lax.fori_loop(1, 8, give, 0)
    lo[tp] = fin[tp]
    fin_all = rc(fin.at[pl.ds(0, 7)], lo.at[pl.ds(0, 7)], send.at[FIN], recv.at[FIN], (fs, tp))
    for j in range(6):
        a2a_desc(j).wait_send()
    for d in started:
        d.wait_send()
    spx_all().wait_send()
    for o in outs:
        o.wait()
    for o in commons:
        o.wait()
    fin_all.wait_recv()
    last = pltpu.make_async_copy(lo, lo_out, loc.at[6])
    last.start()
    fin_all.wait_send()
    last.wait()


def fused(*args):
    any_ = pl.BlockSpec(memory_space=pl.ANY)
    V = pltpu.VMEM
    shape = jax.ShapeDtypeStruct
    return pl.pallas_call(
        kernel,
        out_shape=[shape((8, 32, 256), bf16)] + [shape((32, 64, 128), bf16)] * 3 + [shape((8, 256, 128), bf16)] * 3,
        in_specs=[any_] * 10,
        out_specs=[any_] * 7,
        scratch_shapes=[
            V((256, 2048), bf16),
            V((6, 256), jnp.int32),
            V((6, 256), f32),
            V((1, 64), f32),
            V((3, 32, 64, 128), f32),
            V((3, 64, 128), f32),
            V((3, 32, 64, 128), bf16),
            V((3, 32, 64, 1024), bf16),
            V((8, 128, COLS), bf16),
            V((3, 8, 256, 128), bf16),
            V((256, 2048), bf16),
            V((8, 128, 1024), f32),
            V((8, 128, 1024), bf16),
            V((8, 128, 2048), bf16),
            V((2, 4, 128, 1024), bf16),
            V((3, 32, 1024), bf16),
            V((2, 2, 8, 32, 1024), bf16),
            V((2, 4, 32, 1024), bf16),
            V((128, 1024), bf16),
            V((256, 2048), bf16),
            V((8, 32, 2048), bf16),
            V((8, 32, 256), bf16),
            V((8, 32, 256), bf16),
            pltpu.SemaphoreType.DMA((NSEM,)),
            pltpu.SemaphoreType.DMA((NSEM,)),
            pltpu.SemaphoreType.DMA((10,)),
        ],
        compiler_params=pltpu.CompilerParams(collective_id=0, has_side_effects=True, vmem_limit_bytes=60 * 2**20),
    )(*args)


def settle_kernel(*refs):
    n = (len(refs) - 2) // 3
    ins, outs, held = refs[:n], refs[n : 2 * n], refs[2 * n : 3 * n]
    sem_in, sem_out = refs[-2:]
    get = [pltpu.make_async_copy(ins[k], held[k], sem_in.at[k]) for k in range(n)]
    put = [pltpu.make_async_copy(held[k], outs[k], sem_out.at[k]) for k in range(n)]
    for g in get:
        g.start()
    for k in range(n):
        get[k].wait()
        put[k].start()
    for p in put:
        p.wait()


def settle(*arrays):
    any_ = pl.BlockSpec(memory_space=pl.ANY)
    n = len(arrays)
    return pl.pallas_call(
        settle_kernel,
        out_shape=[jax.ShapeDtypeStruct(a.shape, a.dtype) for a in arrays],
        in_specs=[any_] * n,
        out_specs=[any_] * n,
        scratch_shapes=[pltpu.VMEM(a.shape, a.dtype) for a in arrays]
        + [pltpu.SemaphoreType.DMA((n,)), pltpu.SemaphoreType.DMA((n,))],
        compiler_params=pltpu.CompilerParams(vmem_limit_bytes=60 * 2**20),
    )(*arrays)


def body(tokens, routes, route_weights, norm_gain, *weights):
    lo, sg, su, sd, cg, cu, cd = settle(*fused(tokens, routes.T, route_weights.T, norm_gain.reshape(1, 64), *weights))
    sample = [a.reshape(1, 2048, 128) for a in (sg, su, sd)]
    common = [a.reshape(2048, 128) for a in (cg, cu, cd)]
    return (lo.reshape(256, 256), *sample, *common)


def solution(mesh):
    return jax.shard_map(
        body,
        mesh=mesh,
        in_specs=(P("fs", None), P("fs", None), P("fs", None), P("fs"), P(None, "fs", "tp"), P(None, "fs", "tp"), P(None, "fs", "tp"), P("fs", "tp"), P("fs", "tp"), P("fs", "tp")),
        out_specs=(P("fs", "tp"), P("fs", None, "tp"), P("fs", None, "tp"), P("fs", None, "tp"), P(None, "tp"), P(None, "tp"), P(None, "tp")),
        check_vma=False,
    )
```
